32 devices in a mesh: sp: 8 (over z, x), tp: 4 (over y, core).
Axes of the slice: x: 2, y: 2, z: 4, core: 2. Of those that a mesh axis runs over, the one named last changes fastest.
Arguments:
- tokens_in: bfloat16 [4096, 4096], P(('sp', 'tp')), may hold values from -64 to 64
- w_query: bfloat16 [4096, 2048], P(None, 'tp'), may hold values from -0.09375 to 0.09375
- w_key: bfloat16 [4096, 2048], P(None, 'tp'), may hold values from -0.09375 to 0.09375
- w_value: bfloat16 [4096, 2048], P(None, 'tp'), may hold values from -0.09375 to 0.09375
- w_out: bfloat16 [2048, 4096], P('tp'), may hold values from -1 to 1
Outputs:
- mixed: bfloat16 [4096, 4096], P(('sp', 'tp'))
- log_weight: float32 [32, 4096], P('tp', 'sp')
The draws below stay inside these ranges and needn't reach their ends.
All inputs are finite; a program needn't handle non-finite values.
Results may differ from the reference program's by a relative error of at most 0.019.
Values may be sent and summed in bfloat16 or wider, within the bound.
No kernel may reach another device: no remote copies, remote signals or barrier semaphores. Data moves between devices by JAX's collectives and lax.ppermute only.
A program may use at most 128 MiB of HBM per device.

```python
import jax
import jax.numpy as jnp
from jax import lax

D = 4096
HEADS = 32
HEAD_DIM = 64
SIDE_SPAN = 64
MIDDLE_DILATION = 8
WIDEST_DILATION = 64
TOKENS = 4096
N_TP = 4


def draw_tokens_in(key, part):
    base_key = jax.random.fold_in(jax.random.fold_in(key, 11), 0)
    values = jax.random.truncated_normal(base_key, -4.0, 4.0, (TOKENS, D), jnp.float32)
    return values.astype(jnp.bfloat16)


def steps_of(own_key, extent, cuts, low, high):
    def one(dim, shards_of):
        draws = jax.random.uniform(jax.random.fold_in(jax.random.fold_in(own_key, 6), dim), (shards_of,), jnp.float32, low / len(cuts), high / len(cuts))
        return jnp.repeat(jnp.exp(draws), extent[dim] // shards_of).reshape((-1,) + (1,) * (len(extent) - dim - 1))

    gain = one(*cuts[0])
    for cut in cuts[1:]:
        gain = gain * one(*cut)
    return gain


def gaussian(key, dims, scale, bound, shards=(), kind=jnp.bfloat16):
    entries = scale * jax.random.normal(key, dims, jnp.float32)
    if shards:
        entries = entries * steps_of(key, dims, shards, -0.22, 0.18)
    return jnp.clip(entries, -bound, bound).astype(kind)


def setup_inputs(seed: int = 0) -> dict:
    arg_keys = jax.random.split(jax.random.key(seed), 6)
    tokens_in = draw_tokens_in(jax.random.fold_in(arg_keys[5], 71), 0)
    w_query = gaussian(arg_keys[1], (D, HEADS * HEAD_DIM), D ** -0.5, 0.09375, ((1, 4),))
    w_key = gaussian(arg_keys[2], (D, HEADS * HEAD_DIM), D ** -0.5, 0.09375, ((1, 4),))
    w_value = gaussian(arg_keys[3], (D, HEADS * HEAD_DIM), D ** -0.5, 0.09375, ((1, 4),))
    w_out = gaussian(arg_keys[4], (HEADS * HEAD_DIM, D), HEADS ** -0.5, 1.0, ((0, 4),))
    return {"tokens_in": tokens_in, "w_query": w_query, "w_key": w_key, "w_value": w_value, "w_out": w_out}


ROTARY_BASE = 500000.0
NEGATIVE = -1e30


def rotate(block, positions):
    half_size = block.shape[-1] // 2
    freq = 1.0 / (ROTARY_BASE ** (jnp.arange(half_size, dtype=jnp.float32) / half_size))
    angle = positions[:, None] * freq[None, :]
    cosine = jnp.cos(angle)[:, None, :]
    sine = jnp.sin(angle)[:, None, :]
    front = block[..., :half_size]
    back = block[..., half_size:]
    return jnp.concatenate([front * cosine - back * sine, back * cosine + front * sine], axis=-1)


def pattern_attend(query, keys, values, lead_rows, dilation_step, low_row, high_row):
    rows_total, head_count, head_size = query.shape
    class_len = rows_total // dilation_step
    first_class = lead_rows // dilation_step - SIDE_SPAN
    class_q = query.reshape(class_len, dilation_step, head_count, head_size)
    class_k = keys.reshape(keys.shape[0] // dilation_step, dilation_step, head_count, head_size)
    class_v = values.reshape(values.shape[0] // dilation_step, dilation_step, head_count, head_size)
    sub_k = class_k[first_class:first_class + class_len + 2 * SIDE_SPAN]
    sub_v = class_v[first_class:first_class + class_len + 2 * SIDE_SPAN]
    if class_len <= SIDE_SPAN:
        block_len = class_len
        block_count = 1
        win_k = sub_k[None]
        win_v = sub_v[None]
        blocks_q = class_q[None]
    else:
        block_len = SIDE_SPAN
        block_count = class_len // SIDE_SPAN
        part_k = sub_k.reshape(block_count + 2, SIDE_SPAN, dilation_step, head_count, head_size)
        part_v = sub_v.reshape(block_count + 2, SIDE_SPAN, dilation_step, head_count, head_size)
        win_k = jnp.concatenate([part_k[:-2], part_k[1:-1], part_k[2:]], axis=1)
        win_v = jnp.concatenate([part_v[:-2], part_v[1:-1], part_v[2:]], axis=1)
        blocks_q = class_q.reshape(block_count, SIDE_SPAN, dilation_step, head_count, head_size)
    width = block_len + 2 * SIDE_SPAN
    scores = jnp.einsum('nasht,nksht->nshak', blocks_q, win_k, preferred_element_type=jnp.float32)
    scores = scores * (head_size ** -0.5)
    q_index = jnp.arange(block_len, dtype=jnp.int32)
    k_index = jnp.arange(width, dtype=jnp.int32)
    b_index = jnp.arange(block_count, dtype=jnp.int32)
    s_index = jnp.arange(dilation_step, dtype=jnp.int32)
    in_band = jnp.abs(k_index[None, :] - SIDE_SPAN - q_index[:, None]) <= SIDE_SPAN
    key_position = ((first_class + b_index[:, None] * block_len + k_index[None, :]) * dilation_step)[:, None, :] + s_index[None, :, None]
    is_valid = (key_position >= low_row) & (key_position < high_row)
    keep_mask = in_band[None, None, None] & is_valid[:, :, None, None, :]
    scores = jnp.where(keep_mask, scores, NEGATIVE)
    maxima = jnp.max(scores, axis=-1, keepdims=True)
    expo = jnp.exp(scores - maxima)
    totals = jnp.sum(expo, axis=-1)
    numerator = jnp.einsum('nshak,nksht->nasht', expo.astype(jnp.bfloat16), win_v, preferred_element_type=jnp.float32)
    totals_t = jnp.transpose(totals, (0, 3, 1, 2))
    result = (numerator / totals_t[..., None]).astype(jnp.bfloat16).reshape(rows_total, head_count, head_size)
    log_sum = jnp.transpose(maxima[..., 0] + jnp.log(totals), (0, 3, 1, 2)).reshape(rows_total, head_count)
    return result, log_sum


def combine(results):
    sums = jnp.stack([item[1] for item in results], axis=0)
    peak = jnp.max(sums, axis=0)
    share = jnp.exp(sums - peak[None])
    weight_sum = share[0] + share[1] + share[2]
    accum = share[0][..., None] * results[0][0].astype(jnp.float32)
    accum = accum + share[1][..., None] * results[1][0].astype(jnp.float32)
    accum = accum + share[2][..., None] * results[2][0].astype(jnp.float32)
    attended = (accum / weight_sum[..., None]).astype(jnp.bfloat16)
    return attended, peak + jnp.log(weight_sum)


def reference(tokens_in, w_query, w_key, w_value, w_out):
    positions = jnp.arange(TOKENS, dtype=jnp.float32)
    shape3 = (TOKENS, HEADS, HEAD_DIM)
    query = rotate(jnp.dot(tokens_in, w_query, preferred_element_type=jnp.float32).reshape(shape3), positions).astype(jnp.bfloat16)
    key = rotate(jnp.dot(tokens_in, w_key, preferred_element_type=jnp.float32).reshape(shape3), positions).astype(jnp.bfloat16)
    value = jnp.dot(tokens_in, w_value, preferred_element_type=jnp.float32).astype(jnp.bfloat16).reshape(shape3)
    query_h = jnp.transpose(query, (1, 0, 2))[:, :, None, :]
    key_h = jnp.transpose(key, (1, 0, 2))[:, :, None, :]
    value_h = jnp.transpose(value, (1, 0, 2))[:, :, None, :]

    def one_head(items):
        head_q, head_k, head_v = items
        results = []
        for dilation_step in (1, MIDDLE_DILATION, WIDEST_DILATION):
            border_extent = SIDE_SPAN * dilation_step
            pad_k = jnp.pad(head_k, ((border_extent, border_extent), (0, 0), (0, 0)))
            pad_v = jnp.pad(head_v, ((border_extent, border_extent), (0, 0), (0, 0)))
            results.append(pattern_attend(head_q, pad_k, pad_v, border_extent, dilation_step, border_extent, border_extent + TOKENS))
        attended, log_sum = combine(results)
        return attended[:, 0, :], log_sum[:, 0]

    attended_h, log_weight = lax.map(one_head, (query_h, key_h, value_h))
    attended = jnp.transpose(attended_h, (1, 0, 2)).reshape(TOKENS, HEADS * HEAD_DIM)
    group_cols = HEADS * HEAD_DIM // N_TP
    total = jnp.zeros((TOKENS, D), jnp.float32)
    for group in range(N_TP):
        part = jnp.dot(attended[:, group * group_cols:(group + 1) * group_cols],
                       w_out[group * group_cols:(group + 1) * group_cols], preferred_element_type=jnp.float32)
        rounded = lax.optimization_barrier(part.astype(jnp.bfloat16))
        total = total + rounded.astype(jnp.float32)
    return total.astype(jnp.bfloat16), log_weight
```

```python
import jax
import jax.numpy as jnp
from jax import lax
from jax.experimental import pallas as pl
from jax.experimental.pallas import tpu as pltpu
from jax.sharding import PartitionSpec as P

HEAD_DIM = 64
SIDE_SPAN = 64
MIDDLE_DILATION = 8
WIDEST_DILATION = 64


ROTARY_BASE = 500000.0
NEGATIVE = -1e30


def shifted(block, axis, distance):
    devices = range(lax.axis_size(axis))
    route = [(i - distance, i) for i in devices if i - distance in devices]
    return lax.ppermute(block, axis, route)


def rotate(block, positions):
    half_size = block.shape[-1] // 2
    freq = 1.0 / ROTARY_BASE ** (jnp.arange(half_size, dtype=jnp.float32) / half_size)
    angle = positions[:, None] * freq[None, :]
    cosine = jnp.cos(angle)[:, None, :]
    sine = jnp.sin(angle)[:, None, :]
    front = block[..., :half_size]
    back = block[..., half_size:]
    return jnp.concatenate([front * cosine - back * sine, back * cosine + front * sine], axis=-1)


def pattern_attend(query, keys, values, lead_rows, dilation_step, low_row, high_row):
    rows_total, head_count, head_size = query.shape
    class_len = rows_total // dilation_step
    first_class = lead_rows // dilation_step - SIDE_SPAN
    class_q = query.reshape(class_len, dilation_step, head_count, head_size)
    class_k = keys.reshape(keys.shape[0] // dilation_step, dilation_step, head_count, head_size)
    class_v = values.reshape(values.shape[0] // dilation_step, dilation_step, head_count, head_size)
    sub_k = class_k[first_class : first_class + class_len + 2 * SIDE_SPAN]
    sub_v = class_v[first_class : first_class + class_len + 2 * SIDE_SPAN]
    if class_len <= SIDE_SPAN:
        block_len = class_len
        block_count = 1
        win_k = sub_k[None]
        win_v = sub_v[None]
        blocks_q = class_q[None]
    else:
        block_len = SIDE_SPAN
        block_count = class_len // SIDE_SPAN
        part_k = sub_k.reshape(block_count + 2, SIDE_SPAN, dilation_step, head_count, head_size)
        part_v = sub_v.reshape(block_count + 2, SIDE_SPAN, dilation_step, head_count, head_size)
        win_k = jnp.concatenate([part_k[:-2], part_k[1:-1], part_k[2:]], axis=1)
        win_v = jnp.concatenate([part_v[:-2], part_v[1:-1], part_v[2:]], axis=1)
        blocks_q = class_q.reshape(block_count, SIDE_SPAN, dilation_step, head_count, head_size)
    width = block_len + 2 * SIDE_SPAN
    scores = jnp.einsum("nasht,nksht->nshak", blocks_q, win_k, preferred_element_type=jnp.float32)
    scores = scores * head_size ** (-0.5)
    q_index = jnp.arange(block_len, dtype=jnp.int32)
    k_index = jnp.arange(width, dtype=jnp.int32)
    b_index = jnp.arange(block_count, dtype=jnp.int32)
    s_index = jnp.arange(dilation_step, dtype=jnp.int32)
    in_band = jnp.abs(k_index[None, :] - SIDE_SPAN - q_index[:, None]) <= SIDE_SPAN
    key_position = (
        (first_class + b_index[:, None] * block_len + k_index[None, :]) * dilation_step
    )[:, None, :] + s_index[None, :, None]
    is_valid = (key_position >= low_row) & (key_position < high_row)
    keep_mask = in_band[None, None, None] & is_valid[:, :, None, None, :]
    scores = jnp.where(keep_mask, scores, NEGATIVE)
    maxima = jnp.max(scores, axis=-1, keepdims=True)
    expo = jnp.exp(scores - maxima)
    totals = jnp.sum(expo, axis=-1)
    numerator = jnp.einsum(
        "nshak,nksht->nasht", expo.astype(jnp.bfloat16), win_v, preferred_element_type=jnp.float32
    )
    totals_t = jnp.transpose(totals, (0, 3, 1, 2))
    result = (
        (numerator / totals_t[..., None])
        .astype(jnp.bfloat16)
        .reshape(rows_total, head_count, head_size)
    )
    log_sum = jnp.transpose(maxima[..., 0] + jnp.log(totals), (0, 3, 1, 2)).reshape(
        rows_total, head_count
    )
    return (result, log_sum)


def combine(results):
    sums = jnp.stack([item[1] for item in results], axis=0)
    peak = jnp.max(sums, axis=0)
    share = jnp.exp(sums - peak[None])
    weight_sum = share[0] + share[1] + share[2]
    accum = share[0][..., None] * results[0][0].astype(jnp.float32)
    accum = accum + share[1][..., None] * results[1][0].astype(jnp.float32)
    accum = accum + share[2][..., None] * results[2][0].astype(jnp.float32)
    attended = (accum / weight_sum[..., None]).astype(jnp.bfloat16)
    return (attended, peak + jnp.log(weight_sum))


def general_device(tokens_in, w_query, w_key, w_value, w_out):
    col_count = w_query.shape[1]
    head_count = col_count // HEAD_DIM
    piece = lax.all_gather(tokens_in, "tp", axis=0, tiled=True)
    projected = jnp.concatenate(
        [
            jnp.dot(piece, w_query, preferred_element_type=jnp.float32),
            jnp.dot(piece, w_key, preferred_element_type=jnp.float32),
            jnp.dot(piece, w_value, preferred_element_type=jnp.float32),
        ],
        axis=1,
    )
    rows_total = projected.shape[0]
    sp_size = lax.axis_size("sp")
    sp_place = lax.axis_index("sp")
    positions = (sp_place * rows_total + jnp.arange(rows_total, dtype=jnp.int32)).astype(
        jnp.float32
    )
    shape3 = (rows_total, head_count, HEAD_DIM)
    query = rotate(projected[:, :col_count].reshape(shape3), positions).astype(jnp.bfloat16)
    keys = rotate(projected[:, col_count : 2 * col_count].reshape(shape3), positions).astype(
        jnp.bfloat16
    )
    values = projected[:, 2 * col_count :].astype(jnp.bfloat16).reshape(shape3)
    per_device_span = -(-(SIDE_SPAN * MIDDLE_DILATION) // rows_total)
    earlier_k = []
    earlier_v = []
    before_k, before_v = shifted((keys, values), "sp", 1)
    after_k, after_v = shifted((keys, values), "sp", -1)
    earlier_k.insert(0, before_k)
    earlier_v.insert(0, before_v)
    later_k = [after_k]
    later_v = [after_v]
    key_buf = jnp.concatenate(earlier_k + [keys] + later_k, axis=0)
    value_buf = jnp.concatenate(earlier_v + [values] + later_v, axis=0)
    lead_rows = per_device_span * rows_total
    low_row = lead_rows - sp_place * rows_total
    key_buf, value_buf, lead_rows, low_row, high_row = (
        key_buf,
        value_buf,
        lead_rows,
        low_row,
        low_row + sp_size * rows_total,
    )
    results = [
        pattern_attend(query, key_buf, value_buf, lead_rows, dilation_step, low_row, high_row)
        for dilation_step in (1, MIDDLE_DILATION)
    ]
    class_stride = WIDEST_DILATION // sp_size
    border_extent = SIDE_SPAN * class_stride
    class_shape = (rows_total // sp_size, sp_size, head_count, HEAD_DIM)
    parts = (
        lax.all_to_all(query.reshape(class_shape), "sp", split_axis=1, concat_axis=0, tiled=True),
        lax.all_to_all(keys.reshape(class_shape), "sp", split_axis=1, concat_axis=0, tiled=True),
        lax.all_to_all(values.reshape(class_shape), "sp", split_axis=1, concat_axis=0, tiled=True),
    )
    item_heads = parts[0].shape[2]
    flat = [item.reshape(rows_total, item_heads, HEAD_DIM) for item in parts]
    pad_k = jnp.pad(flat[1], ((border_extent, border_extent), (0, 0), (0, 0)))
    pad_v = jnp.pad(flat[2], ((border_extent, border_extent), (0, 0), (0, 0)))
    result, log_sum = pattern_attend(
        flat[0],
        pad_k,
        pad_v,
        border_extent,
        class_stride,
        border_extent,
        border_extent + rows_total,
    )
    result_back = lax.all_to_all(
        result.reshape(rows_total, 1, item_heads, HEAD_DIM),
        "sp",
        split_axis=0,
        concat_axis=1,
        tiled=True,
    )
    sum_back = lax.all_to_all(
        log_sum.reshape(rows_total, 1, item_heads), "sp", split_axis=0, concat_axis=1, tiled=True
    )
    results.append((result_back.reshape(shape3), sum_back.reshape(rows_total, head_count)))
    attended, log_weight = combine(results)
    flat_out = attended.reshape(rows_total, col_count)
    mixed = lax.psum_scatter(
        jnp.dot(flat_out, w_out, preferred_element_type=jnp.float32).astype(jnp.bfloat16),
        "tp",
        scatter_dimension=0,
        tiled=True,
    )
    return (mixed, jnp.transpose(log_weight, (1, 0)))


LANES = 128


def sin_tables(positions, lanes):
    half_size = HEAD_DIM // 2
    lane = jnp.arange(lanes, dtype=jnp.int32)
    step = (lane % half_size).astype(jnp.float32)
    freq = 1.0 / ROTARY_BASE ** (step / half_size)
    angle = positions.astype(jnp.float32)[:, None] * freq[None, :]
    sign = jnp.where(lane % HEAD_DIM < half_size, -1.0, 1.0)
    return jnp.cos(angle), jnp.sin(angle) * sign[None, :]


def turned(block, cosine, sine):
    rows, width = block.shape
    half_size = HEAD_DIM // 2
    lane = lax.broadcasted_iota(jnp.int32, (rows, width), 1)
    ahead = pltpu.roll(block, width - half_size, 1)
    behind = pltpu.roll(block, half_size, 1)
    other = jnp.where(lane % HEAD_DIM < half_size, ahead, behind)
    reps = width // cosine.shape[1]
    cosine = jnp.concatenate([cosine] * reps, axis=1)
    sine = jnp.concatenate([sine] * reps, axis=1)
    return block * cosine + other * sine


def project_three(xs, wq_ref, wk_ref, wv_ref, cosine, sine):
    scale = HEAD_DIM ** (-0.5)
    q = jnp.dot(xs[...], wq_ref[...], preferred_element_type=jnp.float32)
    q = (turned(q, cosine, sine) * scale).astype(jnp.bfloat16)
    k = jnp.dot(xs[...], wk_ref[...], preferred_element_type=jnp.float32)
    k = turned(k, cosine, sine).astype(jnp.bfloat16)
    v = jnp.dot(xs[...], wv_ref[...], preferred_element_type=jnp.float32)
    return q, k, v.astype(jnp.bfloat16)


def fill_pair(place, mine_ref, peer_ref, xs):
    rows = mine_ref.shape[0]
    core = place[1]
    xs[pl.ds(pl.multiple_of(core * rows, rows), rows), :] = mine_ref[...]
    xs[pl.ds(pl.multiple_of((1 - core) * rows, rows), rows), :] = peer_ref[...]


def near_kernel(place, mine_ref, peer_ref, wq_ref, wk_ref, wv_ref, cos_ref, sin_ref, out_ref, xs):
    @pl.when(pl.program_id(0) == 0)
    def _():
        fill_pair(place, mine_ref, peer_ref, xs)

    parts = project_three(xs, wq_ref, wk_ref, wv_ref, cos_ref[...], sin_ref[...])
    for n in range(3):
        out_ref[n] = parts[n]


def far_kernel(
    place, mine_ref, peer_ref, wq_ref, wk_ref, wv_ref, cos_ref, sin_ref, near_ref,
    nat_ref, send_ref, head_ref, tail_ref, xs, perm,
):
    rows = nat_ref.shape[1]
    half = rows // 2
    classes, _, per_class, _ = send_ref.shape

    @pl.when(pl.program_id(0) == 0)
    def _():
        fill_pair(place, mine_ref, peer_ref, xs)
        target = lax.broadcasted_iota(jnp.int32, (rows, rows), 0)
        source = lax.broadcasted_iota(jnp.int32, (rows, rows), 1)
        wanted = (target % per_class) * classes + target // per_class
        perm[...] = jnp.where(source == wanted, 1.0, 0.0).astype(jnp.bfloat16)

    parts = project_three(xs, wq_ref, wk_ref, wv_ref, cos_ref[...], sin_ref[...])
    row = place[0]
    near_at = pl.multiple_of(row * half, half)
    far_at = pl.multiple_of((1 - row) * half, half)
    for n in range(3):
        nat_ref[n, pl.ds(near_at, half), :] = near_ref[n]
        nat_ref[n, pl.ds(far_at, half), :] = parts[n]
        whole = nat_ref[n]
        moved = jnp.dot(perm[...], whole, preferred_element_type=jnp.float32)
        moved = moved.astype(jnp.bfloat16)
        for c in range(classes):
            send_ref[c, n] = moved[c * per_class : (c + 1) * per_class]
        if n:
            head_ref[n - 1] = nat_ref[n, :SIDE_SPAN, :]
            tail_ref[n - 1] = nat_ref[n, rows - SIDE_SPAN :, :]


def soft_pair(q, k, v, bias):
    lane = lax.broadcasted_iota(jnp.int32, q.shape, 1)
    outs = []
    sums = []
    for h in range(LANES // HEAD_DIM):
        own = (lane // HEAD_DIM) == h
        q_h = jnp.where(own, q, jnp.zeros_like(q))
        s = lax.dot_general(
            q_h, k, (((1,), (1,)), ((), ())), preferred_element_type=jnp.float32
        )
        s = s + bias
        top = jnp.max(s, axis=1, keepdims=True)
        e = jnp.exp(s - top)
        total = jnp.sum(e, axis=1, keepdims=True)
        o = jnp.dot(e.astype(jnp.bfloat16), v, preferred_element_type=jnp.float32)
        outs.append(o / total)
        sums.append(top + jnp.log(total))
    rows = q.shape[0]
    lane = lax.broadcasted_iota(jnp.int32, (rows, LANES), 1)
    result = outs[0]
    for h in range(1, len(outs)):
        result = jnp.where(lane // HEAD_DIM == h, outs[h], result)
    return result, sums


def place_sums(sums, step, rows):
    lane = lax.broadcasted_iota(jnp.int32, (rows, LANES), 1)
    out = jnp.zeros((rows, LANES), jnp.float32)
    for h in range(len(sums)):
        out = jnp.where(lane == step * len(sums) + h, sums[h], out)
    return out


def local_kernel(edge, qkv_ref, before_ref, after_ref, out_ref, lse_ref, ks, vs):
    rows = qkv_ref.shape[1]
    step = pl.program_id(0)
    for n, buf in ((1, ks), (2, vs)):
        buf[:SIDE_SPAN] = before_ref[n - 1]
        buf[SIDE_SPAN : SIDE_SPAN + rows] = qkv_ref[n]
        buf[SIDE_SPAN + rows :] = after_ref[n - 1]
    block = 2 * SIDE_SPAN
    width = block + 2 * SIDE_SPAN
    r = lax.broadcasted_iota(jnp.int32, (block, width), 0)
    c = lax.broadcasted_iota(jnp.int32, (block, width), 1)
    band = jnp.where(jnp.abs(c - SIDE_SPAN - r) <= SIDE_SPAN, 0.0, NEGATIVE)
    first = jnp.where(c < SIDE_SPAN, edge[0].astype(jnp.float32) * NEGATIVE, 0.0)
    last = jnp.where(c >= width - SIDE_SPAN, edge[1].astype(jnp.float32) * NEGATIVE, 0.0)

    @pl.when(step == 0)
    def _():
        lse_ref[...] = jnp.zeros_like(lse_ref)

    count = rows // block
    for b in range(count):
        bias = band
        if b == 0:
            bias = bias + first
        if b == count - 1:
            bias = bias + last
        at = slice(b * block, (b + 1) * block)
        keys = slice(b * block, b * block + width)
        o, sums = soft_pair(qkv_ref[0, at, :], ks[keys], vs[keys], bias)
        out_ref[at, :] = o.astype(jnp.bfloat16)
        lse_ref[at, :] += place_sums(sums, step, block)


def wide_kernel(near_step, far_step, qkv_ref, out_ref, bias, lse):
    sources, _, per, lanes = qkv_ref.shape
    rows = sources * per
    step = pl.program_id(0)
    block = 128

    @pl.when(step == 0)
    def _():
        lse[...] = jnp.zeros_like(lse)
        for b in range(rows // block):
            r = lax.broadcasted_iota(jnp.int32, (block, rows), 0) + b * block
            c = lax.broadcasted_iota(jnp.int32, (block, rows), 1)
            gap = jnp.abs(r - c)
            near = (gap % near_step == 0) & (gap <= SIDE_SPAN * near_step)
            far = (gap % far_step == 0) & (gap <= SIDE_SPAN * far_step)
            one = jnp.where(near | far, 0.0, NEGATIVE)
            bias[b * block : (b + 1) * block] = jnp.where(near & far, jnp.log(2.0), one)

    q = qkv_ref[:, 0].reshape(rows, lanes)
    k = qkv_ref[:, 1].reshape(rows, lanes)
    v = qkv_ref[:, 2].reshape(rows, lanes)
    for b in range(rows // block):
        at = slice(b * block, (b + 1) * block)
        o, sums = soft_pair(q[at], k, v, bias[at])
        first = b * block // per
        o = o.astype(jnp.bfloat16).reshape(block // per, per, lanes)
        lane_at = pl.ds(pl.multiple_of(step * lanes, lanes), lanes)
        out_ref[first : first + block // per, :, lane_at] = o
        lse[at] += place_sums(sums, step, block)

    @pl.when(step == pl.num_programs(0) - 1)
    def _():
        heads = pl.num_programs(0) * (LANES // HEAD_DIM)
        value = lse[...]
        high = value.astype(jnp.bfloat16).astype(jnp.float32)
        middle = (value - high).astype(jnp.bfloat16).astype(jnp.float32)
        low = value - high - middle
        packed = high + pltpu.roll(middle, heads, 1) + pltpu.roll(low, 2 * heads, 1)
        packed = packed.astype(jnp.bfloat16).reshape(sources, per, LANES)
        out_ref[:, :, out_ref.shape[2] - LANES :] = packed


def merge_kernel(tp_place, near_ref, lse_ref, wide_ref, att_ref, lw_ref, flat):
    rows, cols = near_ref.shape
    sources, per, width = wide_ref.shape
    heads = lw_ref.shape[0]
    for c in range(sources):
        flat[c * per : (c + 1) * per] = wide_ref[c]
    block = rows // 4
    lane = lax.broadcasted_iota(jnp.int32, (block, LANES), 1)
    for b in range(rows // block):
        r = lax.broadcasted_iota(jnp.int32, (block, rows), 0) + b * block
        m = lax.broadcasted_iota(jnp.int32, (block, rows), 1)
        pick = jnp.where(m == (r % sources) * per + r // sources, 1.0, 0.0)
        wide = jnp.dot(pick.astype(jnp.bfloat16), flat[...], preferred_element_type=jnp.float32)
        at = slice(b * block, (b + 1) * block)
        parts = wide[:, width - LANES :]
        l_wide = parts + pltpu.roll(parts, LANES - heads, 1)
        l_wide = l_wide + pltpu.roll(parts, LANES - 2 * heads, 1)
        l_near = lse_ref[at, :]
        peak = jnp.maximum(l_near, l_wide)
        s_near = jnp.exp(l_near - peak)
        s_wide = jnp.exp(l_wide - peak)
        total = s_near + s_wide
        lw = peak + jnp.log(total)
        lw_ref[:, at] = jnp.transpose(lw)[:heads]
        w_near = s_near / total
        w_wide = s_wide / total
        slot = 3 - jnp.bitwise_xor(b, tp_place[0])
        to = pl.ds(pl.multiple_of(slot * block, block), block)
        for g in range(cols // LANES):
            h = 2 * g
            even = lane < HEAD_DIM
            a = jnp.where(even, w_near[:, h : h + 1], w_near[:, h + 1 : h + 2])
            z = jnp.where(even, w_wide[:, h : h + 1], w_wide[:, h + 1 : h + 2])
            cut = slice(g * LANES, (g + 1) * LANES)
            o = a * near_ref[at, cut].astype(jnp.float32) + z * wide[:, cut]
            att_ref[to, cut] = o.astype(jnp.bfloat16)


def params(kib=56000):
    return pltpu.CompilerParams(
        vmem_limit_bytes=kib * 1024, dimension_semantics=("arbitrary",)
    )


def cost(flops, size):
    return pl.CostEstimate(flops=int(flops), bytes_accessed=int(size), transcendentals=0)


SCALARS = pl.BlockSpec(memory_space=pltpu.SMEM)


def fast_device(tokens_in, w_query, w_key, w_value, w_out):
    own_rows, depth = tokens_in.shape
    cols = w_query.shape[1]
    heads = cols // HEAD_DIM
    tp_size = lax.axis_size("tp")
    sp_size = lax.axis_size("sp")
    tp_place = lax.axis_index("tp")
    sp_place = lax.axis_index("sp")
    rows = own_rows * tp_size
    half = rows // 2
    per = rows // sp_size
    cross = [(i, i ^ 2) for i in range(tp_size)]
    beside = [(i, i ^ 1) for i in range(tp_size)]
    far_mine = lax.ppermute(tokens_in, "tp", cross)
    near_peer = lax.ppermute(tokens_in, "tp", beside)
    far_peer = lax.ppermute(far_mine, "tp", beside)
    y_place = tp_place // 2
    place = jnp.stack([y_place, tp_place % 2]).astype(jnp.int32)
    span = jnp.arange(half, dtype=jnp.int32)
    base = sp_place * rows
    near_tables = sin_tables(base + y_place * half + span, LANES)
    far_tables = sin_tables(base + (1 - y_place) * half + span, LANES)
    wide_cols = min(256, cols)
    steps = cols // wide_cols
    x_spec = pl.BlockSpec((own_rows, depth), lambda j: (0, 0))
    w_spec = pl.BlockSpec((depth, wide_cols), lambda j: (0, j))
    t_spec = pl.BlockSpec((half, LANES), lambda j: (0, 0))
    near_spec = pl.BlockSpec((3, half, wide_cols), lambda j: (0, 0, j))
    edge_spec = pl.BlockSpec((2, SIDE_SPAN, wide_cols), lambda j: (0, 0, j))
    work = 2 * half * depth * 3 * cols
    moved = 3 * depth * cols * 2
    bf16 = jnp.bfloat16
    near = pl.pallas_call(
        near_kernel,
        grid=(steps,),
        in_specs=[SCALARS, x_spec, x_spec, w_spec, w_spec, w_spec, t_spec, t_spec],
        out_specs=near_spec,
        out_shape=jax.ShapeDtypeStruct((3, half, cols), bf16),
        scratch_shapes=[pltpu.VMEM((half, depth), bf16)],
        compiler_params=params(),
        cost_estimate=cost(work, moved),
        name="near_project",
    )(place, tokens_in, near_peer, w_query, w_key, w_value, *near_tables)
    nat, send, head, tail = pl.pallas_call(
        far_kernel,
        grid=(steps,),
        in_specs=[SCALARS, x_spec, x_spec, w_spec, w_spec, w_spec, t_spec, t_spec, near_spec],
        out_specs=[
            pl.BlockSpec((3, rows, wide_cols), lambda j: (0, 0, j)),
            pl.BlockSpec((sp_size, 3, per, wide_cols), lambda j: (0, 0, 0, j)),
            edge_spec,
            edge_spec,
        ],
        out_shape=[
            jax.ShapeDtypeStruct((3, rows, cols), bf16),
            jax.ShapeDtypeStruct((sp_size, 3, per, cols), bf16),
            jax.ShapeDtypeStruct((2, SIDE_SPAN, cols), bf16),
            jax.ShapeDtypeStruct((2, SIDE_SPAN, cols), bf16),
        ],
        scratch_shapes=[pltpu.VMEM((half, depth), bf16), pltpu.VMEM((rows, rows), bf16)],
        compiler_params=params(),
        cost_estimate=cost(work, moved),
        name="far_project",
    )(place, far_mine, far_peer, w_query, w_key, w_value, *far_tables, near)
    gathered = lax.all_to_all(send, "sp", split_axis=0, concat_axis=0, tiled=True)
    before = shifted(tail, "sp", 1)
    after = shifted(head, "sp", -1)
    edge = jnp.stack([sp_place == 0, sp_place == sp_size - 1]).astype(jnp.int32)
    groups = cols // LANES
    halo_spec = pl.BlockSpec((2, SIDE_SPAN, LANES), lambda j: (0, 0, j))
    o_near, l_near = pl.pallas_call(
        local_kernel,
        grid=(groups,),
        in_specs=[
            SCALARS,
            pl.BlockSpec((3, rows, LANES), lambda j: (0, 0, j)),
            halo_spec,
            halo_spec,
        ],
        out_specs=[
            pl.BlockSpec((rows, LANES), lambda j: (0, j)),
            pl.BlockSpec((rows, LANES), lambda j: (0, 0)),
        ],
        out_shape=[
            jax.ShapeDtypeStruct((rows, cols), bf16),
            jax.ShapeDtypeStruct((rows, LANES), jnp.float32),
        ],
        scratch_shapes=[pltpu.VMEM((rows + 2 * SIDE_SPAN, LANES), bf16)] * 2,
        compiler_params=params(),
        cost_estimate=cost(4e9, 4e6),
        name="local_attend",
    )(edge, nat, before, after)
    wide = pl.pallas_call(
        lambda *refs: wide_kernel(MIDDLE_DILATION // sp_size, WIDEST_DILATION // sp_size, *refs),
        grid=(groups,),
        in_specs=[pl.BlockSpec((sp_size, 3, per, LANES), lambda j: (0, 0, 0, j))],
        out_specs=pl.BlockSpec((sp_size, per, cols + LANES), lambda j: (0, 0, 0)),
        out_shape=jax.ShapeDtypeStruct((sp_size, per, cols + LANES), bf16),
        scratch_shapes=[
            pltpu.VMEM((rows, rows), jnp.float32),
            pltpu.VMEM((rows, LANES), jnp.float32),
        ],
        compiler_params=params(),
        cost_estimate=cost(8e9, 4e6),
        name="wide_attend",
    )(gathered)
    back = lax.all_to_all(wide, "sp", split_axis=0, concat_axis=0, tiled=True)
    whole = pl.BlockSpec(memory_space=pltpu.VMEM)
    attended, log_weight = pl.pallas_call(
        merge_kernel,
        in_specs=[SCALARS, whole, whole, whole],
        out_specs=[whole, whole],
        out_shape=[
            jax.ShapeDtypeStruct((rows, cols), bf16),
            jax.ShapeDtypeStruct((heads, rows), jnp.float32),
        ],
        scratch_shapes=[pltpu.VMEM((rows, cols + LANES), bf16)],
        compiler_params=pltpu.CompilerParams(vmem_limit_bytes=24 * 2**20),
        cost_estimate=cost(2e9, 4e6),
        name="merge",
    )(tp_place.astype(jnp.int32)[None], o_near, l_near, back)

    def product(lo, hi):
        block = attended[lo * own_rows : hi * own_rows]
        return jnp.dot(block, w_out, preferred_element_type=jnp.float32)

    first = lax.ppermute(product(0, 1).astype(bf16), "tp", beside)
    second = (product(1, 2) + first.astype(jnp.float32)).astype(bf16)
    crossed = lax.ppermute(second, "tp", cross)
    third = lax.ppermute(product(2, 3).astype(bf16), "tp", beside)
    total = product(3, 4) + third.astype(jnp.float32)
    mixed = (total + crossed.astype(jnp.float32)).astype(bf16)
    return (mixed, log_weight)


def per_device(tokens_in, w_query, w_key, w_value, w_out):
    sp_size = lax.axis_size("sp")
    tp_size = lax.axis_size("tp")
    rows = tokens_in.shape[0] * tp_size
    fits = (
        tp_size == 4
        and MIDDLE_DILATION % sp_size == 0
        and WIDEST_DILATION % sp_size == 0
        and tokens_in.shape[0] == 2 * SIDE_SPAN
        and (rows // sp_size) % 16 == 0
        and 128 % (rows // sp_size) == 0
        and w_query.shape[1] % 256 == 0
        and 3 * (w_query.shape[1] // HEAD_DIM) <= LANES
    )
    chosen = fast_device if fits else general_device
    return chosen(tokens_in, w_query, w_key, w_value, w_out)


def solution(mesh):
    in_specs = (P(("sp", "tp"), None), P(None, "tp"), P(None, "tp"), P(None, "tp"), P("tp", None))
    out_specs = (P(("sp", "tp"), None), P("tp", "sp"))
    return jax.shard_map(
        per_device, mesh=mesh, in_specs=in_specs, out_specs=out_specs, check_vma=False
    )
```

```python
import jax
import jax.numpy as jnp
from jax import lax
from jax.experimental import pallas as pl
from jax.experimental.pallas import tpu as pltpu
from jax.sharding import PartitionSpec as P

HEAD_DIM = 64
SIDE_SPAN = 64
MIDDLE_DILATION = 8
WIDEST_DILATION = 64


ROTARY_BASE = 500000.0
NEGATIVE = -1e30


def shifted(block, axis, distance):
    devices = range(lax.axis_size(axis))
    route = [(i - distance, i) for i in devices if i - distance in devices]
    return lax.ppermute(block, axis, route)


def rotate(block, positions):
    half_size = block.shape[-1] // 2
    freq = 1.0 / ROTARY_BASE ** (jnp.arange(half_size, dtype=jnp.float32) / half_size)
    angle = positions[:, None] * freq[None, :]
    cosine = jnp.cos(angle)[:, None, :]
    sine = jnp.sin(angle)[:, None, :]
    front = block[..., :half_size]
    back = block[..., half_size:]
    return jnp.concatenate([front * cosine - back * sine, back * cosine + front * sine], axis=-1)


def pattern_attend(query, keys, values, lead_rows, dilation_step, low_row, high_row):
    rows_total, head_count, head_size = query.shape
    class_len = rows_total // dilation_step
    first_class = lead_rows // dilation_step - SIDE_SPAN
    class_q = query.reshape(class_len, dilation_step, head_count, head_size)
    class_k = keys.reshape(keys.shape[0] // dilation_step, dilation_step, head_count, head_size)
    class_v = values.reshape(values.shape[0] // dilation_step, dilation_step, head_count, head_size)
    sub_k = class_k[first_class : first_class + class_len + 2 * SIDE_SPAN]
    sub_v = class_v[first_class : first_class + class_len + 2 * SIDE_SPAN]
    if class_len <= SIDE_SPAN:
        block_len = class_len
        block_count = 1
        win_k = sub_k[None]
        win_v = sub_v[None]
        blocks_q = class_q[None]
    else:
        block_len = SIDE_SPAN
        block_count = class_len // SIDE_SPAN
        part_k = sub_k.reshape(block_count + 2, SIDE_SPAN, dilation_step, head_count, head_size)
        part_v = sub_v.reshape(block_count + 2, SIDE_SPAN, dilation_step, head_count, head_size)
        win_k = jnp.concatenate([part_k[:-2], part_k[1:-1], part_k[2:]], axis=1)
        win_v = jnp.concatenate([part_v[:-2], part_v[1:-1], part_v[2:]], axis=1)
        blocks_q = class_q.reshape(block_count, SIDE_SPAN, dilation_step, head_count, head_size)
    width = block_len + 2 * SIDE_SPAN
    scores = jnp.einsum("nasht,nksht->nshak", blocks_q, win_k, preferred_element_type=jnp.float32)
    scores = scores * head_size ** (-0.5)
    q_index = jnp.arange(block_len, dtype=jnp.int32)
    k_index = jnp.arange(width, dtype=jnp.int32)
    b_index = jnp.arange(block_count, dtype=jnp.int32)
    s_index = jnp.arange(dilation_step, dtype=jnp.int32)
    in_band = jnp.abs(k_index[None, :] - SIDE_SPAN - q_index[:, None]) <= SIDE_SPAN
    key_position = (
        (first_class + b_index[:, None] * block_len + k_index[None, :]) * dilation_step
    )[:, None, :] + s_index[None, :, None]
    is_valid = (key_position >= low_row) & (key_position < high_row)
    keep_mask = in_band[None, None, None] & is_valid[:, :, None, None, :]
    scores = jnp.where(keep_mask, scores, NEGATIVE)
    maxima = jnp.max(scores, axis=-1, keepdims=True)
    expo = jnp.exp(scores - maxima)
    totals = jnp.sum(expo, axis=-1)
    numerator = jnp.einsum(
        "nshak,nksht->nasht", expo.astype(jnp.bfloat16), win_v, preferred_element_type=jnp.float32
    )
    totals_t = jnp.transpose(totals, (0, 3, 1, 2))
    result = (
        (numerator / totals_t[..., None])
        .astype(jnp.bfloat16)
        .reshape(rows_total, head_count, head_size)
    )
    log_sum = jnp.transpose(maxima[..., 0] + jnp.log(totals), (0, 3, 1, 2)).reshape(
        rows_total, head_count
    )
    return (result, log_sum)


def combine(results):
    sums = jnp.stack([item[1] for item in results], axis=0)
    peak = jnp.max(sums, axis=0)
    share = jnp.exp(sums - peak[None])
    weight_sum = share[0] + share[1] + share[2]
    accum = share[0][..., None] * results[0][0].astype(jnp.float32)
    accum = accum + share[1][..., None] * results[1][0].astype(jnp.float32)
    accum = accum + share[2][..., None] * results[2][0].astype(jnp.float32)
    attended = (accum / weight_sum[..., None]).astype(jnp.bfloat16)
    return (attended, peak + jnp.log(weight_sum))


def general_device(tokens_in, w_query, w_key, w_value, w_out):
    col_count = w_query.shape[1]
    head_count = col_count // HEAD_DIM
    piece = lax.all_gather(tokens_in, "tp", axis=0, tiled=True)
    projected = jnp.concatenate(
        [
            jnp.dot(piece, w_query, preferred_element_type=jnp.float32),
            jnp.dot(piece, w_key, preferred_element_type=jnp.float32),
            jnp.dot(piece, w_value, preferred_element_type=jnp.float32),
        ],
        axis=1,
    )
    rows_total = projected.shape[0]
    sp_size = lax.axis_size("sp")
    sp_place = lax.axis_index("sp")
    positions = (sp_place * rows_total + jnp.arange(rows_total, dtype=jnp.int32)).astype(
        jnp.float32
    )
    shape3 = (rows_total, head_count, HEAD_DIM)
    query = rotate(projected[:, :col_count].reshape(shape3), positions).astype(jnp.bfloat16)
    keys = rotate(projected[:, col_count : 2 * col_count].reshape(shape3), positions).astype(
        jnp.bfloat16
    )
    values = projected[:, 2 * col_count :].astype(jnp.bfloat16).reshape(shape3)
    per_device_span = -(-(SIDE_SPAN * MIDDLE_DILATION) // rows_total)
    earlier_k = []
    earlier_v = []
    before_k, before_v = shifted((keys, values), "sp", 1)
    after_k, after_v = shifted((keys, values), "sp", -1)
    earlier_k.insert(0, before_k)
    earlier_v.insert(0, before_v)
    later_k = [after_k]
    later_v = [after_v]
    key_buf = jnp.concatenate(earlier_k + [keys] + later_k, axis=0)
    value_buf = jnp.concatenate(earlier_v + [values] + later_v, axis=0)
    lead_rows = per_device_span * rows_total
    low_row = lead_rows - sp_place * rows_total
    key_buf, value_buf, lead_rows, low_row, high_row = (
        key_buf,
        value_buf,
        lead_rows,
        low_row,
        low_row + sp_size * rows_total,
    )
    results = [
        pattern_attend(query, key_buf, value_buf, lead_rows, dilation_step, low_row, high_row)
        for dilation_step in (1, MIDDLE_DILATION)
    ]
    class_stride = WIDEST_DILATION // sp_size
    border_extent = SIDE_SPAN * class_stride
    class_shape = (rows_total // sp_size, sp_size, head_count, HEAD_DIM)
    parts = (
        lax.all_to_all(query.reshape(class_shape), "sp", split_axis=1, concat_axis=0, tiled=True),
        lax.all_to_all(keys.reshape(class_shape), "sp", split_axis=1, concat_axis=0, tiled=True),
        lax.all_to_all(values.reshape(class_shape), "sp", split_axis=1, concat_axis=0, tiled=True),
    )
    item_heads = parts[0].shape[2]
    flat = [item.reshape(rows_total, item_heads, HEAD_DIM) for item in parts]
    pad_k = jnp.pad(flat[1], ((border_extent, border_extent), (0, 0), (0, 0)))
    pad_v = jnp.pad(flat[2], ((border_extent, border_extent), (0, 0), (0, 0)))
    result, log_sum = pattern_attend(
        flat[0],
        pad_k,
        pad_v,
        border_extent,
        class_stride,
        border_extent,
        border_extent + rows_total,
    )
    result_back = lax.all_to_all(
        result.reshape(rows_total, 1, item_heads, HEAD_DIM),
        "sp",
        split_axis=0,
        concat_axis=1,
        tiled=True,
    )
    sum_back = lax.all_to_all(
        log_sum.reshape(rows_total, 1, item_heads), "sp", split_axis=0, concat_axis=1, tiled=True
    )
    results.append((result_back.reshape(shape3), sum_back.reshape(rows_total, head_count)))
    attended, log_weight = combine(results)
    flat_out = attended.reshape(rows_total, col_count)
    mixed = lax.psum_scatter(
        jnp.dot(flat_out, w_out, preferred_element_type=jnp.float32).astype(jnp.bfloat16),
        "tp",
        scatter_dimension=0,
        tiled=True,
    )
    return (mixed, jnp.transpose(log_weight, (1, 0)))


LANES = 128


def sin_tables(positions, lanes):
    half_size = HEAD_DIM // 2
    lane = jnp.arange(lanes, dtype=jnp.int32)
    step = (lane % half_size).astype(jnp.float32)
    freq = 1.0 / ROTARY_BASE ** (step / half_size)
    angle = positions.astype(jnp.float32)[:, None] * freq[None, :]
    sign = jnp.where(lane % HEAD_DIM < half_size, -1.0, 1.0)
    return jnp.cos(angle), jnp.sin(angle) * sign[None, :]


def turned(block, cosine, sine):
    rows, width = block.shape
    half_size = HEAD_DIM // 2
    lane = lax.broadcasted_iota(jnp.int32, (rows, width), 1)
    ahead = pltpu.roll(block, width - half_size, 1)
    behind = pltpu.roll(block, half_size, 1)
    other = jnp.where(lane % HEAD_DIM < half_size, ahead, behind)
    reps = width // cosine.shape[1]
    cosine = jnp.concatenate([cosine] * reps, axis=1)
    sine = jnp.concatenate([sine] * reps, axis=1)
    return block * cosine + other * sine


def fill_pair(place, mine_ref, peer_ref, xs):
    rows = mine_ref.shape[0]
    core = place[1]
    xs[pl.ds(pl.multiple_of(core * rows, rows), rows), :] = mine_ref[...]
    xs[pl.ds(pl.multiple_of((1 - core) * rows, rows), rows), :] = peer_ref[...]


def low_part(x, size):
    return jnp.bitwise_and(x, size - 1)


def high_part(x, size):
    return jnp.right_shift(x, size.bit_length() - 1)


def project_kernel(
    place, mine_ref, peer_ref, wq_ref, wk_ref, wv_ref, cos_ref, sin_ref, qkv_ref, send_ref, xs,
):
    rows = qkv_ref.shape[1]
    cols = qkv_ref.shape[2]
    classes, _, per_class, _ = send_ref.shape
    fill_pair(place, mine_ref, peer_ref, xs)
    target = lax.broadcasted_iota(jnp.int32, (rows, rows), 0)
    source = lax.broadcasted_iota(jnp.int32, (rows, rows), 1)
    wanted = low_part(target, per_class) * classes + high_part(target, per_class)
    perm = jnp.where(source == wanted, 1.0, 0.0).astype(jnp.bfloat16)
    scale = HEAD_DIM ** (-0.5)
    width = 256
    for at in range(0, cols, width):
        cut = slice(at, at + width)
        for n, w_ref in enumerate((wq_ref, wk_ref, wv_ref)):
            part = jnp.dot(xs[...], w_ref[:, cut], preferred_element_type=jnp.float32)
            if n < 2:
                part = turned(part, cos_ref[...], sin_ref[...])
            if n == 0:
                part = part * scale
            part = part.astype(jnp.bfloat16)
            qkv_ref[n, :, cut] = part
            moved = jnp.dot(perm, part, preferred_element_type=jnp.float32)
            moved = moved.astype(jnp.bfloat16)
            for c in range(classes):
                send_ref[c, n, :, cut] = moved[c * per_class : (c + 1) * per_class]


def soft_pair(q, k, v, bias):
    lane = lax.broadcasted_iota(jnp.int32, q.shape, 1)
    outs = []
    sums = []
    for h in range(LANES // HEAD_DIM):
        own = (lane // HEAD_DIM) == h
        q_h = jnp.where(own, q, jnp.zeros_like(q))
        s = lax.dot_general(
            q_h, k, (((1,), (1,)), ((), ())), preferred_element_type=jnp.float32
        )
        s = s + bias
        top = jnp.max(s, axis=1, keepdims=True)
        e = jnp.exp(s - top)
        total = jnp.sum(e, axis=1, keepdims=True)
        o = jnp.dot(e.astype(jnp.bfloat16), v, preferred_element_type=jnp.float32)
        outs.append(o / total)
        sums.append(top + jnp.log(total))
    rows = q.shape[0]
    lane = lax.broadcasted_iota(jnp.int32, (rows, LANES), 1)
    result = outs[0]
    for h in range(1, len(outs)):
        result = jnp.where(lane // HEAD_DIM == h, outs[h], result)
    return result, sums


def place_sums(sums, step, rows):
    lane = lax.broadcasted_iota(jnp.int32, (rows, LANES), 1)
    out = jnp.zeros((rows, LANES), jnp.float32)
    for h in range(len(sums)):
        out = jnp.where(lane == step * len(sums) + h, sums[h], out)
    return out


def local_kernel(info, near_ref, far_ref, before_ref, after_ref, out_ref, lse_ref, qs, ks, vs):
    half = near_ref.shape[1]
    rows = 2 * half
    step = pl.program_id(0)
    y = info[2]
    near_at = y * half
    far_at = (1 - y) * half
    for n, buf, lead in ((0, qs, 0), (1, ks, SIDE_SPAN), (2, vs, SIDE_SPAN)):
        for at, ref in ((near_at, near_ref), (far_at, far_ref)):
            buf[pl.ds(pl.multiple_of(at + lead, SIDE_SPAN), half), :] = ref[n]
        if n:
            buf[:SIDE_SPAN] = before_ref[n - 1]
            buf[SIDE_SPAN + rows :] = after_ref[n - 1]
    block = 2 * SIDE_SPAN
    width = block + 2 * SIDE_SPAN
    r = lax.broadcasted_iota(jnp.int32, (block, width), 0)
    c = lax.broadcasted_iota(jnp.int32, (block, width), 1)
    band = jnp.where(jnp.abs(c - SIDE_SPAN - r) <= SIDE_SPAN, 0.0, NEGATIVE)
    first = jnp.where(c < SIDE_SPAN, info[0].astype(jnp.float32) * NEGATIVE, 0.0)
    last = jnp.where(c >= width - SIDE_SPAN, info[1].astype(jnp.float32) * NEGATIVE, 0.0)

    @pl.when(step == 0)
    def _():
        lse_ref[...] = jnp.zeros_like(lse_ref)

    count = rows // block
    for b in range(count):
        bias = band
        if b == 0:
            bias = bias + first
        if b == count - 1:
            bias = bias + last
        at = slice(b * block, (b + 1) * block)
        keys = slice(b * block, b * block + width)
        o, sums = soft_pair(qs[at], ks[keys], vs[keys], bias)
        slot = jnp.bitwise_xor(y, b * block // half)
        start = b * block % half
        inner = slice(start, start + block)
        out_ref[slot, inner, :] = o.astype(jnp.bfloat16)
        lse_ref[slot, inner, :] += place_sums(sums, step, block)


def wide_kernel(near_step, far_step, which, first_ref, second_ref, out_ref, bias, lse):
    sources, _, per, lanes = first_ref.shape
    half = sources * per
    step = pl.program_id(0)
    block = 128

    def index_of(x, part):
        return high_part(x, per) * (2 * per) + part * per + low_part(x, per)

    @pl.when(step == 0)
    def _():
        lse[...] = jnp.zeros_like(lse)
        for b in range(half // block):
            r = lax.broadcasted_iota(jnp.int32, (block, half), 0) + b * block
            r = index_of(r, which[0])
            for k in range(2):
                c = lax.broadcasted_iota(jnp.int32, (block, half), 1)
                c = index_of(c, jnp.bitwise_xor(which[0], k))
                gap = jnp.abs(r - c)
                near = (low_part(gap, near_step) == 0) & (gap <= SIDE_SPAN * near_step)
                far = (low_part(gap, far_step) == 0) & (gap <= SIDE_SPAN * far_step)
                one = jnp.where(near | far, 0.0, NEGATIVE)
                both = jnp.where(near & far, jnp.log(2.0), one)
                bias[b * block : (b + 1) * block, k * half : (k + 1) * half] = both

    q = first_ref[:, 0].reshape(half, lanes)
    k = [ref[:, 1].reshape(half, lanes) for ref in (first_ref, second_ref)]
    v = [ref[:, 2].reshape(half, lanes) for ref in (first_ref, second_ref)]
    k = jnp.concatenate(k, axis=0)
    v = jnp.concatenate(v, axis=0)
    for b in range(half // block):
        at = slice(b * block, (b + 1) * block)
        o, sums = soft_pair(q[at], k, v, bias[at])
        first = b * block // per
        o = o.astype(jnp.bfloat16).reshape(block // per, per, lanes)
        lane_at = pl.ds(pl.multiple_of(step * lanes, lanes), lanes)
        out_ref[first : first + block // per, :, lane_at] = o
        lse[at] += place_sums(sums, step, block)

    @pl.when(step == pl.num_programs(0) - 1)
    def _():
        heads = pl.num_programs(0) * (LANES // HEAD_DIM)
        value = lse[...]
        high = value.astype(jnp.bfloat16).astype(jnp.float32)
        middle = (value - high).astype(jnp.bfloat16).astype(jnp.float32)
        low = value - high - middle
        packed = high + pltpu.roll(middle, heads, 1) + pltpu.roll(low, 2 * heads, 1)
        packed = packed.astype(jnp.bfloat16).reshape(sources, per, LANES)
        out_ref[:, :, out_ref.shape[2] - LANES :] = packed


def merge_kernel(part, place, near_ref, lse_ref, wide_ref, att_ref, lw_ref, flat):
    _, rows, cols = near_ref.shape
    sources, per, width = wide_ref.shape
    heads = lw_ref.shape[0]
    for c in range(sources):
        flat[c * per : (c + 1) * per] = wide_ref[c]
    block = rows // 2
    lane = lax.broadcasted_iota(jnp.int32, (block, LANES), 1)
    for b in range(rows // block):
        r = lax.broadcasted_iota(jnp.int32, (block, rows), 0) + b * block
        m = lax.broadcasted_iota(jnp.int32, (block, rows), 1)
        pick = jnp.where(m == low_part(r, sources) * per + high_part(r, sources), 1.0, 0.0)
        wide = jnp.dot(pick.astype(jnp.bfloat16), flat[...], preferred_element_type=jnp.float32)
        at = slice(b * block, (b + 1) * block)
        parts = wide[:, width - LANES :]
        l_wide = parts + pltpu.roll(parts, LANES - heads, 1)
        l_wide = l_wide + pltpu.roll(parts, LANES - 2 * heads, 1)
        l_near = lse_ref[part, at, :]
        peak = jnp.maximum(l_near, l_wide)
        s_near = jnp.exp(l_near - peak)
        s_wide = jnp.exp(l_wide - peak)
        total = s_near + s_wide
        lw = peak + jnp.log(total)
        lw_ref[:, at] = jnp.transpose(lw)[:heads]
        w_near = s_near / total
        w_wide = s_wide / total
        slot = 1 - jnp.bitwise_xor(b, place[1])
        to = pl.ds(pl.multiple_of(slot * block, block), block)
        for g in range(cols // LANES):
            h = 2 * g
            even = lane < HEAD_DIM
            a = jnp.where(even, w_near[:, h : h + 1], w_near[:, h + 1 : h + 2])
            z = jnp.where(even, w_wide[:, h : h + 1], w_wide[:, h + 1 : h + 2])
            cut = slice(g * LANES, (g + 1) * LANES)
            o = a * near_ref[part, at, cut].astype(jnp.float32) + z * wide[:, cut]
            att_ref[to, cut] = o.astype(jnp.bfloat16)


def params(kib=56000):
    return pltpu.CompilerParams(
        vmem_limit_bytes=kib * 1024, dimension_semantics=("arbitrary",)
    )


def cost(flops, size):
    return pl.CostEstimate(flops=int(flops), bytes_accessed=int(size), transcendentals=0)


PROJECT_MIB = 40
SCALARS = pl.BlockSpec(memory_space=pltpu.SMEM)


def fast_device(tokens_in, w_query, w_key, w_value, w_out):
    own_rows, depth = tokens_in.shape
    cols = w_query.shape[1]
    heads = cols // HEAD_DIM
    tp_size = lax.axis_size("tp")
    sp_size = lax.axis_size("sp")
    tp_place = lax.axis_index("tp")
    sp_place = lax.axis_index("sp")
    rows = own_rows * tp_size
    half = rows // 2
    per = rows // sp_size
    cross = [(i, i ^ 2) for i in range(tp_size)]
    beside = [(i, i ^ 1) for i in range(tp_size)]
    far_mine = lax.ppermute(tokens_in, "tp", cross)
    near_peer = lax.ppermute(tokens_in, "tp", beside)
    y_place = tp_place // 2
    place = jnp.stack([y_place, tp_place % 2]).astype(jnp.int32)
    span = jnp.arange(half, dtype=jnp.int32)
    base = sp_place * rows
    near_tables = sin_tables(base + y_place * half + span, LANES)
    far_tables = sin_tables(base + (1 - y_place) * half + span, LANES)
    share = per // 2
    bf16 = jnp.bfloat16
    whole = pl.BlockSpec(memory_space=pltpu.VMEM)

    def project(mine, peer, tables, name):
        return pl.pallas_call(
            project_kernel,
            in_specs=[SCALARS] + [whole] * 7,
            out_specs=[whole, whole],
            out_shape=[
                jax.ShapeDtypeStruct((3, half, cols), bf16),
                jax.ShapeDtypeStruct((sp_size, 3, share, cols), bf16),
            ],
            scratch_shapes=[pltpu.VMEM((half, depth), bf16)],
            compiler_params=pltpu.CompilerParams(vmem_limit_bytes=PROJECT_MIB * 2**20),
            cost_estimate=cost(2 * half * depth * 3 * cols, 3 * depth * cols * 2),
            name=name,
        )(place, mine, peer, w_query, w_key, w_value, *tables)

    def exchange(block):
        shape = block.shape
        flat = block.reshape(shape[0], -1, shape[-1])
        flat = lax.all_to_all(flat, "sp", split_axis=0, concat_axis=0, tiled=True)
        return flat.reshape(shape)

    near, near_send = project(tokens_in, near_peer, near_tables, "near_project")
    near_all = exchange(near_send)
    near, far_mine = lax.optimization_barrier((near, far_mine))
    far_peer = lax.ppermute(far_mine, "tp", beside)
    far, far_send = project(far_mine, far_peer, far_tables, "far_project")
    far_all = exchange(far_send)
    low = jnp.where(y_place == 0, near[1:, :SIDE_SPAN], far[1:, :SIDE_SPAN])
    top = jnp.where(y_place == 0, far[1:, half - SIDE_SPAN :], near[1:, half - SIDE_SPAN :])
    before = shifted(top, "sp", 1)
    after = shifted(low, "sp", -1)
    info = jnp.stack([sp_place == 0, sp_place == sp_size - 1, y_place == 1]).astype(jnp.int32)
    groups = cols // LANES
    halo_spec = pl.BlockSpec((2, SIDE_SPAN, LANES), lambda j: (0, 0, j))
    half_spec = pl.BlockSpec((3, half, LANES), lambda j: (0, 0, j))
    o_near, l_near = pl.pallas_call(
        local_kernel,
        grid=(groups,),
        in_specs=[SCALARS, half_spec, half_spec, halo_spec, halo_spec],
        out_specs=[
            pl.BlockSpec((2, half, LANES), lambda j: (0, 0, j)),
            pl.BlockSpec((2, half, LANES), lambda j: (0, 0, 0)),
        ],
        out_shape=[
            jax.ShapeDtypeStruct((2, half, cols), bf16),
            jax.ShapeDtypeStruct((2, half, LANES), jnp.float32),
        ],
        scratch_shapes=[pltpu.VMEM((rows, LANES), bf16)]
        + [pltpu.VMEM((rows + 2 * SIDE_SPAN, LANES), bf16)] * 2,
        compiler_params=params(16000),
        cost_estimate=cost(6e9, 4e6),
        name="local_attend",
    )(info, near, far, before, after)
    all_spec = pl.BlockSpec((sp_size, 3, share, LANES), lambda j: (0, 0, 0, j))

    def wide(which, first, second, name):
        return pl.pallas_call(
            lambda *refs: wide_kernel(MIDDLE_DILATION // sp_size, WIDEST_DILATION // sp_size, *refs),
            grid=(groups,),
            in_specs=[SCALARS, all_spec, all_spec],
            out_specs=pl.BlockSpec((sp_size, share, cols + LANES), lambda j: (0, 0, 0)),
            out_shape=jax.ShapeDtypeStruct((sp_size, share, cols + LANES), bf16),
            scratch_shapes=[
                pltpu.VMEM((half, rows), jnp.float32),
                pltpu.VMEM((half, LANES), jnp.float32),
            ],
            compiler_params=params(16000),
            cost_estimate=cost(6e9, 4e6),
            name=name,
        )(which.astype(jnp.int32)[None], first, second)

    def merge(part, returned, name):
        return pl.pallas_call(
            lambda *refs: merge_kernel(part, *refs),
            in_specs=[SCALARS, whole, whole, whole],
            out_specs=[whole, whole],
            out_shape=[
                jax.ShapeDtypeStruct((half, cols), bf16),
                jax.ShapeDtypeStruct((heads, half), jnp.float32),
            ],
            scratch_shapes=[pltpu.VMEM((half, cols + LANES), bf16)],
            compiler_params=pltpu.CompilerParams(vmem_limit_bytes=16 * 2**20),
            cost_estimate=cost(2e9, 4e6),
            name=name,
        )(place, o_near, l_near, returned)

    far_wide = wide(1 - y_place, far_all, near_all, "far_wide")
    far_back = exchange(far_wide)
    near_first, near_second, _ = lax.optimization_barrier((near_all, far_all, far_wide))
    near_wide = wide(y_place, near_first, near_second, "near_wide")
    near_back = exchange(near_wide)
    far_att, far_lw = merge(1, far_back, "far_merge")

    def product(block):
        return jnp.dot(block, w_out, preferred_element_type=jnp.float32)

    first = lax.ppermute(product(far_att[:own_rows]).astype(bf16), "tp", beside)
    second = (product(far_att[own_rows:]) + first.astype(jnp.float32)).astype(bf16)
    crossed = lax.ppermute(second, "tp", cross)
    near_back, second = lax.optimization_barrier((near_back, second))
    near_att, near_lw = merge(0, near_back, "near_merge")
    third = lax.ppermute(product(near_att[:own_rows]).astype(bf16), "tp", beside)
    total = product(near_att[own_rows:]) + third.astype(jnp.float32)
    mixed = (total + crossed.astype(jnp.float32)).astype(bf16)
    swap = y_place == 0
    log_weight = jnp.concatenate(
        [jnp.where(swap, near_lw, far_lw), jnp.where(swap, far_lw, near_lw)], axis=1
    )
    return (mixed, log_weight)


def per_device(tokens_in, w_query, w_key, w_value, w_out):
    sp_size = lax.axis_size("sp")
    tp_size = lax.axis_size("tp")
    rows = tokens_in.shape[0] * tp_size
    fits = (
        tp_size == 4
        and MIDDLE_DILATION % sp_size == 0
        and WIDEST_DILATION % sp_size == 0
        and tokens_in.shape[0] == 2 * SIDE_SPAN
        and (rows // sp_size) % 32 == 0
        and 128 % (rows // sp_size) == 0
        and w_query.shape[1] % 256 == 0
        and 3 * (w_query.shape[1] // HEAD_DIM) <= LANES
    )
    chosen = fast_device if fits else general_device
    return chosen(tokens_in, w_query, w_key, w_value, w_out)


def solution(mesh):
    in_specs = (P(("sp", "tp"), None), P(None, "tp"), P(None, "tp"), P(None, "tp"), P("tp", None))
    out_specs = (P(("sp", "tp"), None), P("tp", "sp"))
    return jax.shard_map(
        per_device, mesh=mesh, in_specs=in_specs, out_specs=out_specs, check_vma=False
    )
```

```python
import jax
import jax.numpy as jnp
from jax import lax
from jax.experimental import pallas as pl
from jax.experimental.pallas import tpu as pltpu
from jax.sharding import PartitionSpec as P

HEAD_DIM = 64
SIDE_SPAN = 64
MIDDLE_DILATION = 8
WIDEST_DILATION = 64


ROTARY_BASE = 500000.0
NEGATIVE = -1e30


def shifted(block, axis, distance):
    devices = range(lax.axis_size(axis))
    route = [(i - distance, i) for i in devices if i - distance in devices]
    return lax.ppermute(block, axis, route)


def rotate(block, positions):
    half_size = block.shape[-1] // 2
    freq = 1.0 / ROTARY_BASE ** (jnp.arange(half_size, dtype=jnp.float32) / half_size)
    angle = positions[:, None] * freq[None, :]
    cosine = jnp.cos(angle)[:, None, :]
    sine = jnp.sin(angle)[:, None, :]
    front = block[..., :half_size]
    back = block[..., half_size:]
    return jnp.concatenate([front * cosine - back * sine, back * cosine + front * sine], axis=-1)


def pattern_attend(query, keys, values, lead_rows, dilation_step, low_row, high_row):
    rows_total, head_count, head_size = query.shape
    class_len = rows_total // dilation_step
    first_class = lead_rows // dilation_step - SIDE_SPAN
    class_q = query.reshape(class_len, dilation_step, head_count, head_size)
    class_k = keys.reshape(keys.shape[0] // dilation_step, dilation_step, head_count, head_size)
    class_v = values.reshape(values.shape[0] // dilation_step, dilation_step, head_count, head_size)
    sub_k = class_k[first_class : first_class + class_len + 2 * SIDE_SPAN]
    sub_v = class_v[first_class : first_class + class_len + 2 * SIDE_SPAN]
    if class_len <= SIDE_SPAN:
        block_len = class_len
        block_count = 1
        win_k = sub_k[None]
        win_v = sub_v[None]
        blocks_q = class_q[None]
    else:
        block_len = SIDE_SPAN
        block_count = class_len // SIDE_SPAN
        part_k = sub_k.reshape(block_count + 2, SIDE_SPAN, dilation_step, head_count, head_size)
        part_v = sub_v.reshape(block_count + 2, SIDE_SPAN, dilation_step, head_count, head_size)
        win_k = jnp.concatenate([part_k[:-2], part_k[1:-1], part_k[2:]], axis=1)
        win_v = jnp.concatenate([part_v[:-2], part_v[1:-1], part_v[2:]], axis=1)
        blocks_q = class_q.reshape(block_count, SIDE_SPAN, dilation_step, head_count, head_size)
    width = block_len + 2 * SIDE_SPAN
    scores = jnp.einsum("nasht,nksht->nshak", blocks_q, win_k, preferred_element_type=jnp.float32)
    scores = scores * head_size ** (-0.5)
    q_index = jnp.arange(block_len, dtype=jnp.int32)
    k_index = jnp.arange(width, dtype=jnp.int32)
    b_index = jnp.arange(block_count, dtype=jnp.int32)
    s_index = jnp.arange(dilation_step, dtype=jnp.int32)
    in_band = jnp.abs(k_index[None, :] - SIDE_SPAN - q_index[:, None]) <= SIDE_SPAN
    key_position = (
        (first_class + b_index[:, None] * block_len + k_index[None, :]) * dilation_step
    )[:, None, :] + s_index[None, :, None]
    is_valid = (key_position >= low_row) & (key_position < high_row)
    keep_mask = in_band[None, None, None] & is_valid[:, :, None, None, :]
    scores = jnp.where(keep_mask, scores, NEGATIVE)
    maxima = jnp.max(scores, axis=-1, keepdims=True)
    expo = jnp.exp(scores - maxima)
    totals = jnp.sum(expo, axis=-1)
    numerator = jnp.einsum(
        "nshak,nksht->nasht", expo.astype(jnp.bfloat16), win_v, preferred_element_type=jnp.float32
    )
    totals_t = jnp.transpose(totals, (0, 3, 1, 2))
    result = (
        (numerator / totals_t[..., None])
        .astype(jnp.bfloat16)
        .reshape(rows_total, head_count, head_size)
    )
    log_sum = jnp.transpose(maxima[..., 0] + jnp.log(totals), (0, 3, 1, 2)).reshape(
        rows_total, head_count
    )
    return (result, log_sum)


def combine(results):
    sums = jnp.stack([item[1] for item in results], axis=0)
    peak = jnp.max(sums, axis=0)
    share = jnp.exp(sums - peak[None])
    weight_sum = share[0] + share[1] + share[2]
    accum = share[0][..., None] * results[0][0].astype(jnp.float32)
    accum = accum + share[1][..., None] * results[1][0].astype(jnp.float32)
    accum = accum + share[2][..., None] * results[2][0].astype(jnp.float32)
    attended = (accum / weight_sum[..., None]).astype(jnp.bfloat16)
    return (attended, peak + jnp.log(weight_sum))


def general_device(tokens_in, w_query, w_key, w_value, w_out):
    col_count = w_query.shape[1]
    head_count = col_count // HEAD_DIM
    piece = lax.all_gather(tokens_in, "tp", axis=0, tiled=True)
    projected = jnp.concatenate(
        [
            jnp.dot(piece, w_query, preferred_element_type=jnp.float32),
            jnp.dot(piece, w_key, preferred_element_type=jnp.float32),
            jnp.dot(piece, w_value, preferred_element_type=jnp.float32),
        ],
        axis=1,
    )
    rows_total = projected.shape[0]
    sp_size = lax.axis_size("sp")
    sp_place = lax.axis_index("sp")
    positions = (sp_place * rows_total + jnp.arange(rows_total, dtype=jnp.int32)).astype(
        jnp.float32
    )
    shape3 = (rows_total, head_count, HEAD_DIM)
    query = rotate(projected[:, :col_count].reshape(shape3), positions).astype(jnp.bfloat16)
    keys = rotate(projected[:, col_count : 2 * col_count].reshape(shape3), positions).astype(
        jnp.bfloat16
    )
    values = projected[:, 2 * col_count :].astype(jnp.bfloat16).reshape(shape3)
    per_device_span = -(-(SIDE_SPAN * MIDDLE_DILATION) // rows_total)
    earlier_k = []
    earlier_v = []
    before_k, before_v = shifted((keys, values), "sp", 1)
    after_k, after_v = shifted((keys, values), "sp", -1)
    earlier_k.insert(0, before_k)
    earlier_v.insert(0, before_v)
    later_k = [after_k]
    later_v = [after_v]
    key_buf = jnp.concatenate(earlier_k + [keys] + later_k, axis=0)
    value_buf = jnp.concatenate(earlier_v + [values] + later_v, axis=0)
    lead_rows = per_device_span * rows_total
    low_row = lead_rows - sp_place * rows_total
    key_buf, value_buf, lead_rows, low_row, high_row = (
        key_buf,
        value_buf,
        lead_rows,
        low_row,
        low_row + sp_size * rows_total,
    )
    results = [
        pattern_attend(query, key_buf, value_buf, lead_rows, dilation_step, low_row, high_row)
        for dilation_step in (1, MIDDLE_DILATION)
    ]
    class_stride = WIDEST_DILATION // sp_size
    border_extent = SIDE_SPAN * class_stride
    class_shape = (rows_total // sp_size, sp_size, head_count, HEAD_DIM)
    parts = (
        lax.all_to_all(query.reshape(class_shape), "sp", split_axis=1, concat_axis=0, tiled=True),
        lax.all_to_all(keys.reshape(class_shape), "sp", split_axis=1, concat_axis=0, tiled=True),
        lax.all_to_all(values.reshape(class_shape), "sp", split_axis=1, concat_axis=0, tiled=True),
    )
    item_heads = parts[0].shape[2]
    flat = [item.reshape(rows_total, item_heads, HEAD_DIM) for item in parts]
    pad_k = jnp.pad(flat[1], ((border_extent, border_extent), (0, 0), (0, 0)))
    pad_v = jnp.pad(flat[2], ((border_extent, border_extent), (0, 0), (0, 0)))
    result, log_sum = pattern_attend(
        flat[0],
        pad_k,
        pad_v,
        border_extent,
        class_stride,
        border_extent,
        border_extent + rows_total,
    )
    result_back = lax.all_to_all(
        result.reshape(rows_total, 1, item_heads, HEAD_DIM),
        "sp",
        split_axis=0,
        concat_axis=1,
        tiled=True,
    )
    sum_back = lax.all_to_all(
        log_sum.reshape(rows_total, 1, item_heads), "sp", split_axis=0, concat_axis=1, tiled=True
    )
    results.append((result_back.reshape(shape3), sum_back.reshape(rows_total, head_count)))
    attended, log_weight = combine(results)
    flat_out = attended.reshape(rows_total, col_count)
    mixed = lax.psum_scatter(
        jnp.dot(flat_out, w_out, preferred_element_type=jnp.float32).astype(jnp.bfloat16),
        "tp",
        scatter_dimension=0,
        tiled=True,
    )
    return (mixed, jnp.transpose(log_weight, (1, 0)))


LANES = 128


def sin_tables(positions, lanes):
    half_size = HEAD_DIM // 2
    lane = jnp.arange(lanes, dtype=jnp.int32)
    step = (lane % half_size).astype(jnp.float32)
    freq = 1.0 / ROTARY_BASE ** (step / half_size)
    angle = positions.astype(jnp.float32)[:, None] * freq[None, :]
    sign = jnp.where(lane % HEAD_DIM < half_size, -1.0, 1.0)
    return jnp.cos(angle), jnp.sin(angle) * sign[None, :]


def turned(block, cosine, sine):
    rows, width = block.shape
    half_size = HEAD_DIM // 2
    lane = lax.broadcasted_iota(jnp.int32, (rows, width), 1)
    ahead = pltpu.roll(block, width - half_size, 1)
    behind = pltpu.roll(block, half_size, 1)
    other = jnp.where(lane % HEAD_DIM < half_size, ahead, behind)
    reps = width // cosine.shape[1]
    cosine = jnp.concatenate([cosine] * reps, axis=1)
    sine = jnp.concatenate([sine] * reps, axis=1)
    return block * cosine + other * sine


def low_part(x, size):
    return jnp.bitwise_and(x, size - 1)


def high_part(x, size):
    return jnp.right_shift(x, size.bit_length() - 1)


def finish_kernel(place, *refs):
    mine_refs, peer_refs = refs[:3], refs[3:6]
    cos_ref, sin_ref, qkv_ref, send_ref = refs[6:]
    rows = qkv_ref.shape[1]
    block = rows // 2
    classes, _, per_class, _ = send_ref.shape
    for refs_of, core in ((mine_refs, place[1]), (peer_refs, 1 - place[1])):
        at = pl.ds(pl.multiple_of(core * block, block), block)
        for n in range(3):
            part = refs_of[n][...]
            if n < 2:
                part = turned(part, cos_ref[at, :], sin_ref[at, :])
            if n == 0:
                part = part * HEAD_DIM ** (-0.5)
            qkv_ref[n, at, :] = part.astype(jnp.bfloat16)
    target = lax.broadcasted_iota(jnp.int32, (rows, rows), 0)
    source = lax.broadcasted_iota(jnp.int32, (rows, rows), 1)
    wanted = low_part(target, per_class) * classes + high_part(target, per_class)
    perm = jnp.where(source == wanted, 1.0, 0.0).astype(jnp.bfloat16)
    for n in range(3):
        moved = jnp.dot(perm, qkv_ref[n], preferred_element_type=jnp.float32)
        moved = moved.astype(jnp.bfloat16)
        for c in range(classes):
            send_ref[c, n] = moved[c * per_class : (c + 1) * per_class]


def soft_pair(q, k, v, bias):
    lane = lax.broadcasted_iota(jnp.int32, q.shape, 1)
    outs = []
    sums = []
    for h in range(LANES // HEAD_DIM):
        own = (lane // HEAD_DIM) == h
        q_h = jnp.where(own, q, jnp.zeros_like(q))
        s = lax.dot_general(
            q_h, k, (((1,), (1,)), ((), ())), preferred_element_type=jnp.float32
        )
        s = s + bias
        top = jnp.max(s, axis=1, keepdims=True)
        e = jnp.exp(s - top)
        total = jnp.sum(e, axis=1, keepdims=True)
        o = jnp.dot(e.astype(jnp.bfloat16), v, preferred_element_type=jnp.float32)
        outs.append(o / total)
        sums.append(top + jnp.log(total))
    rows = q.shape[0]
    lane = lax.broadcasted_iota(jnp.int32, (rows, LANES), 1)
    result = outs[0]
    for h in range(1, len(outs)):
        result = jnp.where(lane // HEAD_DIM == h, outs[h], result)
    return result, sums


def place_sums(sums, step, rows):
    lane = lax.broadcasted_iota(jnp.int32, (rows, LANES), 1)
    out = jnp.zeros((rows, LANES), jnp.float32)
    for h in range(len(sums)):
        out = jnp.where(lane == step * len(sums) + h, sums[h], out)
    return out


def local_kernel(info, near_ref, far_ref, before_ref, after_ref, out_ref, lse_ref, qs, ks, vs):
    half = near_ref.shape[1]
    rows = 2 * half
    step = pl.program_id(0)
    y = info[2]
    near_at = y * half
    far_at = (1 - y) * half
    for n, buf, lead in ((0, qs, 0), (1, ks, SIDE_SPAN), (2, vs, SIDE_SPAN)):
        for at, ref in ((near_at, near_ref), (far_at, far_ref)):
            buf[pl.ds(pl.multiple_of(at + lead, SIDE_SPAN), half), :] = ref[n]
        if n:
            buf[:SIDE_SPAN] = before_ref[n - 1]
            buf[SIDE_SPAN + rows :] = after_ref[n - 1]
    block = 2 * SIDE_SPAN
    width = block + 2 * SIDE_SPAN
    r = lax.broadcasted_iota(jnp.int32, (block, width), 0)
    c = lax.broadcasted_iota(jnp.int32, (block, width), 1)
    band = jnp.where(jnp.abs(c - SIDE_SPAN - r) <= SIDE_SPAN, 0.0, NEGATIVE)
    first = jnp.where(c < SIDE_SPAN, info[0].astype(jnp.float32) * NEGATIVE, 0.0)
    last = jnp.where(c >= width - SIDE_SPAN, info[1].astype(jnp.float32) * NEGATIVE, 0.0)

    @pl.when(step == 0)
    def _():
        lse_ref[...] = jnp.zeros_like(lse_ref)

    count = rows // block
    for b in range(count):
        bias = band
        if b == 0:
            bias = bias + first
        if b == count - 1:
            bias = bias + last
        at = slice(b * block, (b + 1) * block)
        keys = slice(b * block, b * block + width)
        o, sums = soft_pair(qs[at], ks[keys], vs[keys], bias)
        slot = jnp.bitwise_xor(y, b * block // half)
        start = b * block % half
        inner = slice(start, start + block)
        out_ref[slot, inner, :] = o.astype(jnp.bfloat16)
        lse_ref[slot, inner, :] += place_sums(sums, step, block)


def wide_kernel(near_step, far_step, which, first_ref, second_ref, out_ref, bias, lse):
    sources, _, per, lanes = first_ref.shape
    half = sources * per
    step = pl.program_id(0)
    block = 128

    def index_of(x, part):
        return high_part(x, per) * (2 * per) + part * per + low_part(x, per)

    @pl.when(step == 0)
    def _():
        lse[...] = jnp.zeros_like(lse)
        for b in range(half // block):
            r = lax.broadcasted_iota(jnp.int32, (block, half), 0) + b * block
            r = index_of(r, which[0])
            for k in range(2):
                c = lax.broadcasted_iota(jnp.int32, (block, half), 1)
                c = index_of(c, jnp.bitwise_xor(which[0], k))
                gap = jnp.abs(r - c)
                near = (low_part(gap, near_step) == 0) & (gap <= SIDE_SPAN * near_step)
                far = (low_part(gap, far_step) == 0) & (gap <= SIDE_SPAN * far_step)
                one = jnp.where(near | far, 0.0, NEGATIVE)
                both = jnp.where(near & far, jnp.log(2.0), one)
                bias[b * block : (b + 1) * block, k * half : (k + 1) * half] = both

    q = first_ref[:, 0].reshape(half, lanes)
    k = [ref[:, 1].reshape(half, lanes) for ref in (first_ref, second_ref)]
    v = [ref[:, 2].reshape(half, lanes) for ref in (first_ref, second_ref)]
    k = jnp.concatenate(k, axis=0)
    v = jnp.concatenate(v, axis=0)
    for b in range(half // block):
        at = slice(b * block, (b + 1) * block)
        o, sums = soft_pair(q[at], k, v, bias[at])
        first = b * block // per
        o = o.astype(jnp.bfloat16).reshape(block // per, per, lanes)
        lane_at = pl.ds(pl.multiple_of(step * lanes, lanes), lanes)
        out_ref[first : first + block // per, :, lane_at] = o
        lse[at] += place_sums(sums, step, block)

    @pl.when(step == pl.num_programs(0) - 1)
    def _():
        heads = pl.num_programs(0) * (LANES // HEAD_DIM)
        value = lse[...]
        high = value.astype(jnp.bfloat16).astype(jnp.float32)
        middle = (value - high).astype(jnp.bfloat16).astype(jnp.float32)
        low = value - high - middle
        packed = high + pltpu.roll(middle, heads, 1) + pltpu.roll(low, 2 * heads, 1)
        packed = packed.astype(jnp.bfloat16).reshape(sources, per, LANES)
        out_ref[:, :, out_ref.shape[2] - LANES :] = packed


def merge_kernel(part, place, near_ref, lse_ref, wide_ref, att_ref, lw_ref, flat):
    _, rows, cols = near_ref.shape
    sources, per, width = wide_ref.shape
    heads = lw_ref.shape[0]
    for c in range(sources):
        flat[c * per : (c + 1) * per] = wide_ref[c]
    block = rows // 2
    lane = lax.broadcasted_iota(jnp.int32, (block, LANES), 1)
    for b in range(rows // block):
        r = lax.broadcasted_iota(jnp.int32, (block, rows), 0) + b * block
        m = lax.broadcasted_iota(jnp.int32, (block, rows), 1)
        pick = jnp.where(m == low_part(r, sources) * per + high_part(r, sources), 1.0, 0.0)
        wide = jnp.dot(pick.astype(jnp.bfloat16), flat[...], preferred_element_type=jnp.float32)
        at = slice(b * block, (b + 1) * block)
        parts = wide[:, width - LANES :]
        l_wide = parts + pltpu.roll(parts, LANES - heads, 1)
        l_wide = l_wide + pltpu.roll(parts, LANES - 2 * heads, 1)
        l_near = lse_ref[part, at, :]
        peak = jnp.maximum(l_near, l_wide)
        s_near = jnp.exp(l_near - peak)
        s_wide = jnp.exp(l_wide - peak)
        total = s_near + s_wide
        lw = peak + jnp.log(total)
        lw_ref[:, at] = jnp.transpose(lw)[:heads]
        w_near = s_near / total
        w_wide = s_wide / total
        slot = 1 - jnp.bitwise_xor(b, place[1])
        to = pl.ds(pl.multiple_of(slot * block, block), block)
        for g in range(cols // LANES):
            h = 2 * g
            even = lane < HEAD_DIM
            a = jnp.where(even, w_near[:, h : h + 1], w_near[:, h + 1 : h + 2])
            z = jnp.where(even, w_wide[:, h : h + 1], w_wide[:, h + 1 : h + 2])
            cut = slice(g * LANES, (g + 1) * LANES)
            o = a * near_ref[part, at, cut].astype(jnp.float32) + z * wide[:, cut]
            att_ref[to, cut] = o.astype(jnp.bfloat16)


def params(kib=56000):
    return pltpu.CompilerParams(
        vmem_limit_bytes=kib * 1024, dimension_semantics=("arbitrary",)
    )


def cost(flops, size):
    return pl.CostEstimate(flops=int(flops), bytes_accessed=int(size), transcendentals=0)


SCALARS = pl.BlockSpec(memory_space=pltpu.SMEM)


def fast_device(tokens_in, w_query, w_key, w_value, w_out):
    own_rows, depth = tokens_in.shape
    cols = w_query.shape[1]
    heads = cols // HEAD_DIM
    tp_size = lax.axis_size("tp")
    sp_size = lax.axis_size("sp")
    tp_place = lax.axis_index("tp")
    sp_place = lax.axis_index("sp")
    rows = own_rows * tp_size
    half = rows // 2
    per = rows // sp_size
    cross = [(i, i ^ 2) for i in range(tp_size)]
    beside = [(i, i ^ 1) for i in range(tp_size)]
    far_mine = lax.ppermute(tokens_in, "tp", cross)
    near_peer = lax.ppermute(tokens_in, "tp", beside)
    y_place = tp_place // 2
    place = jnp.stack([y_place, tp_place % 2]).astype(jnp.int32)
    span = jnp.arange(half, dtype=jnp.int32)
    base = sp_place * rows
    near_tables = sin_tables(base + y_place * half + span, LANES)
    far_tables = sin_tables(base + (1 - y_place) * half + span, LANES)
    share = per // 2
    bf16 = jnp.bfloat16
    whole = pl.BlockSpec(memory_space=pltpu.VMEM)

    def project(x):
        weights = (w_query, w_key, w_value)
        return [jnp.dot(x, w, preferred_element_type=jnp.float32) for w in weights]

    def finish(mine, peer, tables, name):
        return pl.pallas_call(
            finish_kernel,
            in_specs=[SCALARS] + [whole] * 8,
            out_specs=[whole, whole],
            out_shape=[
                jax.ShapeDtypeStruct((3, half, cols), bf16),
                jax.ShapeDtypeStruct((sp_size, 3, share, cols), bf16),
            ],
            compiler_params=pltpu.CompilerParams(vmem_limit_bytes=16 * 2**20),
            cost_estimate=cost(2e9, 3 * half * cols * 10),
            name=name,
        )(place, *mine, *peer, *tables)

    def exchange(block):
        shape = block.shape
        flat = block.reshape(shape[0], -1, shape[-1])
        flat = lax.all_to_all(flat, "sp", split_axis=0, concat_axis=0, tiled=True)
        return flat.reshape(shape)

    near, near_send = finish(project(tokens_in), project(near_peer), near_tables, "near_finish")
    near_all = exchange(near_send)
    near, far_mine = lax.optimization_barrier((near, far_mine))
    far_peer = lax.ppermute(far_mine, "tp", beside)
    far, far_send = finish(project(far_mine), project(far_peer), far_tables, "far_finish")
    far_all = exchange(far_send)
    low = jnp.where(y_place == 0, near[1:, :SIDE_SPAN], far[1:, :SIDE_SPAN])
    top = jnp.where(y_place == 0, far[1:, half - SIDE_SPAN :], near[1:, half - SIDE_SPAN :])
    before = shifted(top, "sp", 1)
    after = shifted(low, "sp", -1)
    info = jnp.stack([sp_place == 0, sp_place == sp_size - 1, y_place == 1]).astype(jnp.int32)
    groups = cols // LANES
    halo_spec = pl.BlockSpec((2, SIDE_SPAN, LANES), lambda j: (0, 0, j))
    half_spec = pl.BlockSpec((3, half, LANES), lambda j: (0, 0, j))
    o_near, l_near = pl.pallas_call(
        local_kernel,
        grid=(groups,),
        in_specs=[SCALARS, half_spec, half_spec, halo_spec, halo_spec],
        out_specs=[
            pl.BlockSpec((2, half, LANES), lambda j: (0, 0, j)),
            pl.BlockSpec((2, half, LANES), lambda j: (0, 0, 0)),
        ],
        out_shape=[
            jax.ShapeDtypeStruct((2, half, cols), bf16),
            jax.ShapeDtypeStruct((2, half, LANES), jnp.float32),
        ],
        scratch_shapes=[pltpu.VMEM((rows, LANES), bf16)]
        + [pltpu.VMEM((rows + 2 * SIDE_SPAN, LANES), bf16)] * 2,
        compiler_params=params(16000),
        cost_estimate=cost(6e9, 4e6),
        name="local_attend",
    )(info, near, far, before, after)
    all_spec = pl.BlockSpec((sp_size, 3, share, LANES), lambda j: (0, 0, 0, j))

    def wide(which, first, second, name):
        return pl.pallas_call(
            lambda *refs: wide_kernel(MIDDLE_DILATION // sp_size, WIDEST_DILATION // sp_size, *refs),
            grid=(groups,),
            in_specs=[SCALARS, all_spec, all_spec],
            out_specs=pl.BlockSpec((sp_size, share, cols + LANES), lambda j: (0, 0, 0)),
            out_shape=jax.ShapeDtypeStruct((sp_size, share, cols + LANES), bf16),
            scratch_shapes=[
                pltpu.VMEM((half, rows), jnp.float32),
                pltpu.VMEM((half, LANES), jnp.float32),
            ],
            compiler_params=params(16000),
            cost_estimate=cost(6e9, 4e6),
            name=name,
        )(which.astype(jnp.int32)[None], first, second)

    def merge(part, returned, name):
        return pl.pallas_call(
            lambda *refs: merge_kernel(part, *refs),
            in_specs=[SCALARS, whole, whole, whole],
            out_specs=[whole, whole],
            out_shape=[
                jax.ShapeDtypeStruct((half, cols), bf16),
                jax.ShapeDtypeStruct((heads, half), jnp.float32),
            ],
            scratch_shapes=[pltpu.VMEM((half, cols + LANES), bf16)],
            compiler_params=pltpu.CompilerParams(vmem_limit_bytes=16 * 2**20),
            cost_estimate=cost(2e9, 4e6),
            name=name,
        )(place, o_near, l_near, returned)

    far_all, near_all, o_near, l_near = lax.optimization_barrier((far_all, near_all, o_near, l_near))
    far_wide = wide(1 - y_place, far_all, near_all, "far_wide")
    far_back = exchange(far_wide)
    near_first, near_second, _ = lax.optimization_barrier((near_all, far_all, far_wide))
    near_wide = wide(y_place, near_first, near_second, "near_wide")
    far_back, near_wide = lax.optimization_barrier((far_back, near_wide))
    far_att, far_lw = merge(1, far_back, "far_merge")

    def product(block):
        return jnp.dot(block, w_out, preferred_element_type=jnp.float32)

    first = lax.ppermute(product(far_att[:own_rows]).astype(bf16), "tp", beside)
    second = (product(far_att[own_rows:]) + first.astype(jnp.float32)).astype(bf16)
    near_wide, second = lax.optimization_barrier((near_wide, second))
    crossed = lax.ppermute(second, "tp", cross)
    near_back = exchange(near_wide)
    near_att, near_lw = merge(0, near_back, "near_merge")
    third = lax.ppermute(product(near_att[:own_rows]).astype(bf16), "tp", beside)
    total = product(near_att[own_rows:]) + third.astype(jnp.float32)
    mixed = (total + crossed.astype(jnp.float32)).astype(bf16)
    swap = y_place == 0
    log_weight = jnp.concatenate(
        [jnp.where(swap, near_lw, far_lw), jnp.where(swap, far_lw, near_lw)], axis=1
    )
    return (mixed, log_weight)


def per_device(tokens_in, w_query, w_key, w_value, w_out):
    sp_size = lax.axis_size("sp")
    tp_size = lax.axis_size("tp")
    rows = tokens_in.shape[0] * tp_size
    fits = (
        tp_size == 4
        and MIDDLE_DILATION % sp_size == 0
        and WIDEST_DILATION % sp_size == 0
        and tokens_in.shape[0] == 2 * SIDE_SPAN
        and (rows // sp_size) % 32 == 0
        and 128 % (rows // sp_size) == 0
        and w_query.shape[1] % 256 == 0
        and 3 * (w_query.shape[1] // HEAD_DIM) <= LANES
    )
    chosen = fast_device if fits else general_device
    return chosen(tokens_in, w_query, w_key, w_value, w_out)


def solution(mesh):
    in_specs = (P(("sp", "tp"), None), P(None, "tp"), P(None, "tp"), P(None, "tp"), P("tp", None))
    out_specs = (P(("sp", "tp"), None), P("tp", "sp"))
    return jax.shard_map(
        per_device, mesh=mesh, in_specs=in_specs, out_specs=out_specs, check_vma=False
    )
```
